32 devices in a mesh: sp: 16 (over z, y, x), tp: 2 (over core).
Axes of the slice: x: 2, y: 2, z: 4, core: 2. Of those that a mesh axis runs over, the one named last changes fastest.
Arguments:
- stream: bfloat16 [2048, 2048], P('sp', 'tp'), may hold values from -14 to 14
- queries: bfloat16 [2048, 2048], P('sp', 'tp'), may hold values from -6 to 6
- key_rows: bfloat16 [2048, 2048], P('sp', 'tp'), may hold values from -6 to 6
- values: bfloat16 [2048, 2048], P('sp', 'tp'), may hold values from -6 to 6
- out_gate: bfloat16 [2048, 2048], P('sp', 'tp'), may hold values from -6 to 6
- in_gate: float32 [16, 2048], P('tp', 'sp'), may hold values from -4 to 120
- forget_gate: float32 [16, 2048], P('tp', 'sp'), may hold values from -1 to 20
- head_gain: float32 [2048], P('tp'), may hold values from 0.1 to 1.9
- w_out: bfloat16 [2048, 2048], P('tp'), may hold values from -0.30935922 to 0.30935922
- norm_gains: bfloat16 [3, 2048], P(None, 'tp'), may hold values from 0.099609375 to 1.8984375
- w_gate: bfloat16 [2048, 5632], P('sp', 'tp'), may hold values from -0.125 to 0.125
- w_up: bfloat16 [2048, 5632], P('sp', 'tp'), may hold values from -0.125 to 0.125
- w_down: bfloat16 [5632, 2048], P('tp', 'sp'), may hold values from -0.18655063 to 0.18655063
Outputs:
- result: bfloat16 [2048, 2048], P('sp', 'tp')
The draws below stay inside these ranges and needn't reach their ends.
All inputs are finite; a program needn't handle non-finite values.
Results may differ from the reference program's by a relative error of at most 0.012.
Values may be sent and summed in bfloat16 or wider, within the bound.
No kernel may reach another device: no remote copies, remote signals or barrier semaphores. Data moves between devices by JAX's collectives and lax.ppermute only.
A program may use at most 128 MiB of HBM per device.

```python
import jax
import jax.numpy as jnp
from jax import lax

D = 2048
HEADS = 16
HD = 128
FF = 5632
BLOCK = 128
TOK_DEV = 128
TOKENS = 2048
N_SP = 16
N_TP = 2


def draw_in_gate(key, part):
    base_key = jax.random.fold_in(jax.random.fold_in(key, 7), 0)
    values_in = jnp.clip(jax.random.normal(base_key, (HEADS, TOKENS), jnp.float32), -4.0, 4.0)
    return values_in


def draw_forget_gate(key, part):
    rate_key, block_key, jitter_key = jax.random.split(jax.random.fold_in(key, 11), 3)
    fast_share = 0.5
    quick = jax.random.uniform(rate_key, (HEADS,)) < fast_share
    base_rate = jnp.where(quick, 0.02, 0.5 / TOKENS)
    factor = jnp.exp(jax.random.uniform(block_key, (HEADS, TOKENS // BLOCK), jnp.float32, -1.0, 1.0))
    step_rate = jnp.repeat(base_rate[:, None] * factor, BLOCK, axis=1)
    jitter = jnp.clip(0.6 * jax.random.normal(jitter_key, (HEADS, TOKENS), jnp.float32), -2.5, 2.5)
    return -jnp.log(step_rate) + jitter


def column_scales(key):
    levels = jnp.exp(jnp.linspace(-1.2, 1.2, N_TP).astype(jnp.float32))
    order = jax.random.permutation(key, N_TP)
    return jnp.repeat(levels[order], D // N_TP)


def scaled_matrix(key, rows, spread):
    scale_key, entry_key = jax.random.split(key)
    entries = jnp.clip(jax.random.normal(entry_key, (rows, D), jnp.float32), -4.0, 4.0)
    return entries * spread * column_scales(scale_key)[None, :]


def draw_stream(key, part):
    return scaled_matrix(jax.random.fold_in(key, 21), TOKENS, 1.0).astype(jnp.bfloat16)


def draw_w_out(key, part):
    return scaled_matrix(jax.random.fold_in(key, 23), HEADS * HD, (HEADS * HD) ** (-0.5)).astype(jnp.bfloat16)


def draw_w_down(key, part):
    return scaled_matrix(jax.random.fold_in(key, 29), FF, FF ** (-0.5)).astype(jnp.bfloat16)


def shard_levels(own_key, shape, cuts, smallest, largest):
    def one(position, shards_of):
        steps = jax.random.uniform(jax.random.fold_in(jax.random.fold_in(own_key, 6), position), (shards_of,), jnp.float32, smallest / len(cuts), largest / len(cuts))
        return jnp.repeat(jnp.exp(steps), shape[position] // shards_of).reshape((-1,) + (1,) * (len(shape) - position - 1))

    level = one(*cuts[0])
    for cut in cuts[1:]:
        level = level * one(*cut)
    return level


def normal_values(stream_key, dims, deviation, most, cuts=(), kind=jnp.bfloat16):
    factor_of = shard_levels(stream_key, dims, cuts, -0.22, 0.18) if cuts else 1.0
    values = jax.random.normal(stream_key, dims, jnp.float32) * deviation * factor_of
    return jnp.minimum(jnp.maximum(values, -most), most).astype(kind)


def setup_inputs(seed: int = 0) -> dict:
    keys = jax.random.split(jax.random.key(seed), 14)
    stream = draw_stream(jax.random.fold_in(keys[13], 71), 0)
    queries = normal_values(keys[1], (TOKENS, HEADS * HD), 1.0, 6.0, ((0, 16), (1, 2)))
    key_rows = normal_values(keys[2], (TOKENS, HEADS * HD), 1.0, 6.0, ((0, 16), (1, 2)))
    values = normal_values(keys[3], (TOKENS, HEADS * HD), 1.0, 6.0, ((0, 16), (1, 2)))
    out_gate = normal_values(keys[4], (TOKENS, HEADS * HD), 1.0, 6.0, ((0, 16), (1, 2)))
    in_gate = draw_in_gate(jax.random.fold_in(keys[13], 71), 0)
    forget_gate = draw_forget_gate(jax.random.fold_in(keys[13], 71), 0)
    head_gain = jnp.clip(1.0 + 0.18 * jax.random.normal(keys[7], (HEADS * HD,), jnp.float32), 0.1, 1.9)
    w_out = draw_w_out(jax.random.fold_in(keys[13], 71), 0)
    norm_gains = jnp.clip(1.0 + 0.18 * jax.random.normal(keys[9], (3, D), jnp.float32), 0.099609375, 1.8984375).astype(jnp.bfloat16)
    w_gate = normal_values(keys[10], (D, FF), D ** -0.5, 0.125, ((0, 16), (1, 2)))
    w_up = normal_values(keys[11], (D, FF), D ** -0.5, 0.125, ((0, 16), (1, 2)))
    w_down = draw_w_down(jax.random.fold_in(keys[13], 71), 0)
    return dict(stream=stream, queries=queries, key_rows=key_rows, values=values, out_gate=out_gate, in_gate=in_gate, forget_gate=forget_gate, head_gain=head_gain, w_out=w_out, norm_gains=norm_gains, w_gate=w_gate, w_up=w_up, w_down=w_down)


EPS = 1e-06

def cell_outputs(queries, key_rows, values, in_gate, forget_gate):
    highest = lax.Precision.HIGHEST
    blocks = TOKENS // BLOCK
    key_scale = HD ** (-0.5)

    def to_blocks(array):
        return array.astype(jnp.float32).reshape(blocks, BLOCK, HEADS, HD).transpose(0, 2, 1, 3)
    query_all = to_blocks(queries)
    key_all = to_blocks(key_rows) * key_scale
    value_all = to_blocks(values)
    forget_all = jax.nn.log_sigmoid(forget_gate).reshape(HEADS, blocks, BLOCK).transpose(1, 0, 2)
    input_all = in_gate.reshape(HEADS, blocks, BLOCK).transpose(1, 0, 2)
    causal = jnp.tril(jnp.ones((BLOCK, BLOCK), dtype=bool))

    def advance(carried, inputs):
        memory, stabil = carried
        query_blk, key_blk, value_blk, forget_blk, input_blk = inputs
        cumulative = jnp.cumsum(forget_blk, axis=-1)
        within = jnp.where(causal, cumulative[:, :, None] - cumulative[:, None, :] + input_blk[:, None, :], -jnp.inf)
        across = cumulative + stabil[:, None]
        stable = jnp.maximum(across, lax.optimization_barrier(jnp.max(within, axis=-1)))
        weight_in = jnp.exp(within - stable[:, :, None])
        weight_out = jnp.exp(across - stable)
        scores = jnp.einsum('htd,hsd->hts', query_blk, key_blk, precision=highest) * weight_in
        probs_low = lax.optimization_barrier(scores.astype(jnp.bfloat16)).astype(jnp.float32)
        output = jnp.einsum('hts,hsd->htd', probs_low, value_blk, precision=highest)
        output = output + weight_out[:, :, None] * jnp.einsum('htd,hde->hte', query_blk, memory, precision=highest)
        last_sum = cumulative[:, -1]
        toward = last_sum[:, None] - cumulative + input_blk
        stabil_new = jnp.maximum(last_sum + stabil, lax.optimization_barrier(jnp.max(toward, axis=-1)))
        decay_now = jnp.exp(last_sum + stabil - stabil_new)
        weight_key = jnp.exp(toward - stabil_new[:, None])
        weighted = key_blk * weight_key[:, :, None]
        memory_new = decay_now[:, None, None] * memory + jnp.einsum('hsd,hse->hde', weighted, value_blk, precision=highest)
        return ((memory_new, stabil_new), output)
    initial = (jnp.zeros((HEADS, HD, HD), jnp.float32), jnp.zeros((HEADS,), jnp.float32))
    _, outputs = lax.scan(advance, initial, (query_all, key_all, value_all, forget_all, input_all))
    return outputs.transpose(0, 2, 1, 3).reshape(TOKENS, HEADS, HD)

def reference(stream, queries, key_rows, values, out_gate, in_gate, forget_gate, head_gain, w_out, norm_gains, w_gate, w_up, w_down):
    cell = cell_outputs(queries, key_rows, values, in_gate, forget_gate)
    normed_cell = cell * lax.rsqrt(lax.optimization_barrier(jnp.mean(cell * cell, axis=-1, keepdims=True)) + EPS)
    mixed = (normed_cell.reshape(TOKENS, HEADS * HD) * head_gain * jax.nn.sigmoid(out_gate.astype(jnp.float32))).astype(jnp.bfloat16)
    gain_rows = norm_gains.astype(jnp.float32)
    mix_width = HEADS * HD // N_TP
    ffn_width = FF // N_TP

    def rows_block(inputs):
        mixed_rows, stream_rows = inputs
        mix_sum = jnp.zeros((TOK_DEV, D), jnp.float32)
        for member in range(N_TP):
            product = jnp.dot(mixed_rows[:, member * mix_width:(member + 1) * mix_width], w_out[member * mix_width:(member + 1) * mix_width], preferred_element_type=jnp.float32)
            mix_sum = mix_sum + lax.optimization_barrier(product.astype(jnp.bfloat16)).astype(jnp.float32)
        mix_norm = mix_sum * lax.rsqrt(lax.optimization_barrier(jnp.mean(mix_sum * mix_sum, axis=-1, keepdims=True)) + EPS) * gain_rows[0]
        after_low = (stream_rows.astype(jnp.float32) + mix_norm).astype(jnp.bfloat16)
        after_mix = lax.optimization_barrier(after_low).astype(jnp.float32)
        normed = (after_mix * lax.rsqrt(lax.optimization_barrier(jnp.mean(after_mix * after_mix, axis=-1, keepdims=True)) + EPS) * gain_rows[1]).astype(jnp.bfloat16)
        gate_sum = jnp.dot(normed, w_gate, preferred_element_type=jnp.float32)
        up_sum = jnp.dot(normed, w_up, preferred_element_type=jnp.float32)
        hidden = (jax.nn.silu(gate_sum) * up_sum).astype(jnp.bfloat16)
        ffn_sum = jnp.zeros((TOK_DEV, D), jnp.float32)
        for member in range(N_TP):
            product = jnp.dot(hidden[:, member * ffn_width:(member + 1) * ffn_width], w_down[member * ffn_width:(member + 1) * ffn_width], preferred_element_type=jnp.float32)
            ffn_sum = ffn_sum + lax.optimization_barrier(product.astype(jnp.bfloat16)).astype(jnp.float32)
        ffn_norm = ffn_sum * lax.rsqrt(lax.optimization_barrier(jnp.mean(ffn_sum * ffn_sum, axis=-1, keepdims=True)) + EPS) * gain_rows[2]
        return (after_mix + 0.5 * ffn_norm).astype(jnp.bfloat16)
    result = lax.map(rows_block, (mixed.reshape(N_SP, TOK_DEV, HEADS * HD), stream.reshape(N_SP, TOK_DEV, D)))
    return result.reshape(TOKENS, D)
```

```python
import jax
import jax.numpy as jnp
from jax import lax
from jax.sharding import PartitionSpec as P

BLOCK = 128
EPS = 1e-06


def split_axis(n):
    slow = max(d for d in range(1, n + 1) if n % d == 0 and d * d <= n)
    return slow, n // slow


def slow_shift(value, slow, fast, shift, wrap=True):
    pairs = [
        (z * fast + p, (z + shift) % slow * fast + p)
        for z in range(slow)
        for p in range(fast)
        if wrap or 0 <= z + shift < slow
    ]
    return lax.ppermute(value, "sp", pairs)


def fast_swap(value, slow, fast, mask):
    pairs = [(i, i // fast * fast + (i % fast ^ mask)) for i in range(slow * fast)]
    return lax.ppermute(value, "sp", pairs)


def tp_gather(value, axis):
    peers = lax.axis_size("tp")
    if peers != 2:
        return lax.all_gather(value, "tp", axis=axis, tiled=True)
    other = lax.ppermute(value, "tp", [(0, 1), (1, 0)])
    first = lax.axis_index("tp") == 0
    return jnp.concatenate(
        [jnp.where(first, value, other), jnp.where(first, other, value)], axis=axis
    )


def tp_total(value):
    peers = lax.axis_size("tp")
    total = value.astype(jnp.float32)
    for shift in range(1, peers):
        other = lax.ppermute(value, "tp", [(i, (i + shift) % peers) for i in range(peers)])
        total = total + other.astype(jnp.float32)
    return total


def tp_scatter(value, axis):
    peers = lax.axis_size("tp")
    me = lax.axis_index("tp")
    width = value.shape[axis] // peers

    def part(k):
        return lax.dynamic_slice_in_dim(value, k % peers * width, width, axis)

    total = part(me).astype(jnp.float32)
    for shift in range(1, peers):
        other = lax.ppermute(
            part(me + shift), "tp", [(i, (i + shift) % peers) for i in range(peers)]
        )
        total = total + other.astype(jnp.float32)
    return total


def unswap(parts, position):
    parts = list(parts)
    bit = 1
    while bit < len(parts):
        odd = (position & bit) != 0
        parts = [jnp.where(odd, parts[i ^ bit], parts[i]) for i in range(len(parts))]
        bit *= 2
    return parts


def join_states(earlier, later):
    total_early, summit_early, memory_early = earlier
    total_late, summit_late, memory_late = later
    summit = jnp.maximum(total_late + summit_early, summit_late)
    scale_early = jnp.exp(total_late + summit_early - summit)
    scale_late = jnp.exp(summit_late - summit)
    memory = scale_early[:, None, None] * memory_early + scale_late[:, None, None] * memory_late
    return (total_early + total_late, summit, memory)


def pack_state(state):
    total, summit, memory = state
    heads, rows, width = memory.shape
    marks = jnp.zeros((8, width), jnp.float32)
    marks = marks.at[0, :heads].set(total).at[1, :heads].set(summit)
    return jnp.concatenate([memory.reshape(heads * rows, width), marks], axis=0)


def unpack_state(packed, heads):
    width = packed.shape[1]
    memory = packed[:-8].reshape(heads, -1, width)
    return packed[-8, :heads], packed[-7, :heads], memory


def carried_in(state, slow, fast):
    total, summit, memory = state
    heads, rows, width = memory.shape
    position = lax.axis_index("sp")
    line, spot = position // fast, position % fast
    slices = memory.reshape(heads, fast, rows // fast, width).transpose(1, 0, 2, 3)

    def own_slice(k):
        return (total, summit, lax.dynamic_index_in_dim(slices, k, 0, keepdims=False))

    packets = [pack_state(own_slice(spot ^ mask)) for mask in range(fast)]
    packets = [packets[0]] + [fast_swap(packets[m], slow, fast, m) for m in range(1, fast)]
    states = [unpack_state(packet, heads) for packet in unswap(packets, spot)]
    nothing = (
        jnp.zeros_like(total),
        jnp.full_like(summit, -1e30),
        jnp.zeros_like(states[0][2]),
    )
    before = [nothing]
    for one in states:
        before.append(join_states(before[-1], one))
    whole = pack_state(before[-1])
    prior = nothing
    for shift in range(slow - 1, 0, -1):
        came = unpack_state(slow_shift(whole, slow, fast, shift, wrap=False), heads)
        joined = join_states(prior, came)
        prior = jax.tree.map(lambda a, b: jnp.where(line >= shift, a, b), joined, prior)
    answers = jnp.stack([pack_state(join_states(prior, one)) for one in before[:-1]])

    def answer(k):
        return lax.dynamic_index_in_dim(answers, k, 0, keepdims=False)

    back = [answer(spot)] + [
        fast_swap(answer(spot ^ mask), slow, fast, mask) for mask in range(1, fast)
    ]
    back = [unpack_state(packet, heads) for packet in unswap(back, spot)]
    return back[0][0], back[0][1], jnp.concatenate([one[2] for one in back], axis=1)


def cell_block(queries, key_rows, values, in_gate, forget_gate, slow, fast):
    highest = lax.Precision.HIGHEST
    tokens_here = queries.shape[0]
    heads = in_gate.shape[0]
    head_dim = queries.shape[1] // heads
    blocks = tokens_here // BLOCK
    key_scale = head_dim ** (-0.5)
    log_forget = jax.nn.log_sigmoid(forget_gate)
    cumulative = jnp.cumsum(log_forget, axis=1)
    total_log = cumulative[:, -1]
    toward = total_log[:, None] - cumulative + in_gate
    summit = jnp.max(toward, axis=1)
    weight_key = jnp.exp(toward - summit[:, None])
    key_scaled = key_rows.astype(jnp.float32).reshape(tokens_here, heads, head_dim) * key_scale
    value_float = values.astype(jnp.float32).reshape(tokens_here, heads, head_dim)
    weighted = key_scaled * weight_key.T[:, :, None]
    memory_dev = jnp.einsum("shd,she->hde", weighted, value_float, precision=highest)
    prior_total, prior_summit, prior_memory = carried_in(
        (total_log, summit, memory_dev), slow, fast
    )
    stabil = jnp.maximum(prior_total, prior_summit)
    memory = jnp.exp(prior_summit - stabil)[:, None, None] * prior_memory
    causal = jnp.tril(jnp.ones((BLOCK, BLOCK), dtype=bool))
    outputs = []
    for block in range(blocks):
        at = slice(block * BLOCK, (block + 1) * BLOCK)
        query_blk = queries[at].reshape(BLOCK, heads, head_dim)
        key_blk = key_rows[at].reshape(BLOCK, heads, head_dim)
        value_blk = values[at].reshape(BLOCK, heads, head_dim)
        input_blk = in_gate[:, at]
        cumul_blk = jnp.cumsum(log_forget[:, at], axis=-1)
        within = jnp.where(
            causal, cumul_blk[:, :, None] - cumul_blk[:, None, :] + input_blk[:, None, :], -jnp.inf
        )
        inner = jnp.max(within, axis=-1)
        raw_scores = (
            jnp.einsum("thd,shd->hts", query_blk, key_blk, preferred_element_type=jnp.float32)
            * key_scale
        )
        probs_low = (raw_scores * jnp.exp(within - inner[:, :, None])).astype(jnp.bfloat16)
        inside = jnp.einsum("hts,shd->thd", probs_low, value_blk, preferred_element_type=jnp.float32)
        across = cumul_blk + stabil[:, None]
        stable = jnp.maximum(across, inner)
        weight_in = jnp.exp(inner - stable)
        weight_out = jnp.exp(across - stable)
        output = weight_in.T[:, :, None] * inside + weight_out.T[:, :, None] * jnp.einsum(
            "thd,hde->the", query_blk.astype(jnp.float32), memory, precision=highest
        )
        outputs.append(output)
        if block + 1 < blocks:
            last_sum = cumul_blk[:, -1]
            toward_blk = last_sum[:, None] - cumul_blk + input_blk
            stabil_new = jnp.maximum(last_sum + stabil, jnp.max(toward_blk, axis=-1))
            weight_blk = jnp.exp(toward_blk - stabil_new[:, None])
            weighted_blk = key_scaled[at] * weight_blk.T[:, :, None]
            memory = jnp.exp(last_sum + stabil - stabil_new)[:, None, None] * memory + jnp.einsum(
                "shd,she->hde", weighted_blk, value_float[at], precision=highest
            )
            stabil = stabil_new
    return jnp.concatenate(outputs, axis=0)


def spread(block_of, slow, fast):
    line = lax.axis_index("sp") // fast
    pieces = [block_of(line)]
    for shift in range(1, slow):
        pieces.append(slow_shift(block_of((line + shift) % slow), slow, fast, shift))
    groups = [list(range(0, slow, 2)), list(range(1, slow, 2))]
    orders = []
    bits = []
    bit = 1
    while bit < fast:
        bits.append(bit)
        bit *= 2
    for route, group in enumerate(groups):
        held = {0: jnp.stack([pieces[s] for s in group])}
        for bit in bits if route == 0 else bits[::-1]:
            for mask in list(held):
                held[mask ^ bit] = fast_swap(held[mask], slow, fast, bit)
        for mask, value in held.items():
            for k, s in enumerate(group):
                orders.append((s, mask, value[k]))
    return orders


def by_source(pieces, slow, fast):
    position = lax.axis_index("sp")
    line, spot = position // fast, position % fast
    first = pieces[0][2]
    whole = jnp.zeros((slow * fast,) + first.shape, first.dtype)
    for shift, mask, value in pieces:
        source = (line - shift) % slow * fast + (spot ^ mask)
        whole = lax.dynamic_update_index_in_dim(whole, value, source, 0)
    return whole


def shards(
    stream,
    queries,
    key_rows,
    values,
    out_gate,
    in_gate,
    forget_gate,
    head_gain,
    w_out,
    norm_gains,
    w_gate,
    w_up,
    w_down,
):
    slow, fast = split_axis(lax.axis_size("sp"))
    tokens_here = queries.shape[0]
    own_width = stream.shape[1]
    units = w_gate.shape[1] // slow
    rows_in = w_gate.shape[0]
    columns_out = w_down.shape[1]
    n_sp = slow * fast
    tp_at = lax.axis_index("tp")

    def own_half(value, axis):
        return lax.dynamic_slice_in_dim(value, tp_at * own_width, own_width, axis)

    def column_chunk(weight):
        chunks = weight.reshape(rows_in, slow, units).transpose(1, 0, 2)
        return lambda k: lax.dynamic_index_in_dim(chunks, k, 0, keepdims=False)

    gate_pieces = spread(column_chunk(w_gate), slow, fast)
    up_pieces = spread(column_chunk(w_up), slow, fast)
    down_pieces = spread(
        lambda k: lax.dynamic_slice_in_dim(w_down, k * units, units, 0), slow, fast
    )

    stream_full = tp_gather(stream, 1)
    gains_full = tp_gather(norm_gains, 1).astype(jnp.float32)

    cell = cell_block(queries, key_rows, values, in_gate, forget_gate, slow, fast)
    normed_cell = cell * lax.rsqrt(jnp.mean(cell * cell, axis=-1, keepdims=True) + EPS)
    mixed = (
        normed_cell.reshape(tokens_here, -1)
        * head_gain
        * jax.nn.sigmoid(out_gate.astype(jnp.float32))
    ).astype(jnp.bfloat16)
    partial_mix = jnp.dot(mixed, w_out, preferred_element_type=jnp.float32)
    mix_sum = tp_total(partial_mix.astype(jnp.bfloat16))
    mix_norm = (
        mix_sum
        * lax.rsqrt(jnp.mean(mix_sum * mix_sum, axis=1, keepdims=True) + EPS)
        * gains_full[0]
    )
    after_mix = (stream_full.astype(jnp.float32) + mix_norm).astype(jnp.bfloat16)
    kept_rows = after_mix.astype(jnp.float32)
    normed = (
        kept_rows
        * lax.rsqrt(jnp.mean(kept_rows * kept_rows, axis=1, keepdims=True) + EPS)
        * gains_full[1]
    ).astype(jnp.bfloat16)

    normed_half = own_half(normed, 1)
    arrived = [slow_shift(normed_half, slow, fast, shift) for shift in range(1, slow)]
    others = tp_gather(jnp.concatenate(arrived, axis=0), 1)
    normed_all = jnp.concatenate([normed, others], axis=0)

    gate_rows = by_source(gate_pieces, slow, fast).reshape(n_sp * rows_in, units)
    up_rows = by_source(up_pieces, slow, fast).reshape(n_sp * rows_in, units)
    down_rows = by_source(down_pieces, slow, fast)
    gate_part = jnp.dot(normed_all, gate_rows, preferred_element_type=jnp.float32)
    up_part = jnp.dot(normed_all, up_rows, preferred_element_type=jnp.float32)
    hidden = (jax.nn.silu(gate_part) * up_part).astype(jnp.bfloat16)
    down_full = down_rows.transpose(1, 0, 2).reshape(units, n_sp * columns_out)
    ffn_terms = jnp.dot(hidden, down_full, preferred_element_type=jnp.float32)
    ffn_lines = tp_scatter(ffn_terms.astype(jnp.bfloat16), 1)
    ffn_low = ffn_lines.astype(jnp.bfloat16)
    ffn_sum = ffn_lines[:tokens_here]
    for shift in range(1, slow):
        block = ffn_low[shift * tokens_here : (shift + 1) * tokens_here]
        ffn_sum = ffn_sum + slow_shift(block, slow, fast, -shift).astype(jnp.float32)
    ffn_squares = lax.psum(jnp.sum(ffn_sum * ffn_sum, axis=1), "tp")
    width = own_width * lax.axis_size("tp")
    ffn_norm = (
        ffn_sum
        * lax.rsqrt(ffn_squares / width + EPS)[:, None]
        * norm_gains[2].astype(jnp.float32)
    )
    return (own_half(kept_rows, 1) + 0.5 * ffn_norm).astype(jnp.bfloat16)


def solution(mesh):
    in_specs = (
        P("sp", "tp"),
        P("sp", "tp"),
        P("sp", "tp"),
        P("sp", "tp"),
        P("sp", "tp"),
        P("tp", "sp"),
        P("tp", "sp"),
        P("tp"),
        P("tp", None),
        P(None, "tp"),
        P("sp", "tp"),
        P("sp", "tp"),
        P("tp", "sp"),
    )
    out_specs = P("sp", "tp")
    return jax.shard_map(shards, mesh=mesh, in_specs=in_specs, out_specs=out_specs, check_vma=False)
```

```python
import jax
import jax.numpy as jnp
from jax import lax
from jax.experimental import pallas as pl
from jax.experimental.pallas import tpu as pltpu
from jax.sharding import PartitionSpec as P

BLOCK = 128
EPS = 1e-06


def split_axis(n):
    slow = max(d for d in range(1, n + 1) if n % d == 0 and d * d <= n)
    return slow, n // slow


def slow_shift(value, slow, fast, shift, wrap=True):
    pairs = [
        (z * fast + p, (z + shift) % slow * fast + p)
        for z in range(slow)
        for p in range(fast)
        if wrap or 0 <= z + shift < slow
    ]
    return lax.ppermute(value, "sp", pairs)


def fast_swap(value, slow, fast, mask):
    pairs = [(i, i // fast * fast + (i % fast ^ mask)) for i in range(slow * fast)]
    return lax.ppermute(value, "sp", pairs)


def tp_gather(value, axis):
    peers = lax.axis_size("tp")
    if peers != 2:
        return lax.all_gather(value, "tp", axis=axis, tiled=True)
    other = lax.ppermute(value, "tp", [(0, 1), (1, 0)])
    first = lax.axis_index("tp") == 0
    return jnp.concatenate(
        [jnp.where(first, value, other), jnp.where(first, other, value)], axis=axis
    )


def tp_total(value):
    peers = lax.axis_size("tp")
    total = value.astype(jnp.float32)
    for shift in range(1, peers):
        other = lax.ppermute(value, "tp", [(i, (i + shift) % peers) for i in range(peers)])
        total = total + other.astype(jnp.float32)
    return total


def tp_scatter(value, axis):
    peers = lax.axis_size("tp")
    me = lax.axis_index("tp")
    width = value.shape[axis] // peers

    def part(k):
        return lax.dynamic_slice_in_dim(value, k % peers * width, width, axis)

    total = part(me).astype(jnp.float32)
    for shift in range(1, peers):
        other = lax.ppermute(
            part(me + shift), "tp", [(i, (i + shift) % peers) for i in range(peers)]
        )
        total = total + other.astype(jnp.float32)
    return total


def unswap(parts, position):
    parts = list(parts)
    bit = 1
    while bit < len(parts):
        odd = (position & bit) != 0
        parts = [jnp.where(odd, parts[i ^ bit], parts[i]) for i in range(len(parts))]
        bit *= 2
    return parts


def join_states(earlier, later):
    total_early, summit_early, memory_early = earlier
    total_late, summit_late, memory_late = later
    summit = jnp.maximum(total_late + summit_early, summit_late)
    scale_early = jnp.exp(total_late + summit_early - summit)
    scale_late = jnp.exp(summit_late - summit)
    memory = scale_early[:, None, None] * memory_early + scale_late[:, None, None] * memory_late
    return (total_early + total_late, summit, memory)


def pack_state(state):
    total, summit, memory = state
    heads, rows, width = memory.shape
    marks = jnp.zeros((8, width), jnp.float32)
    marks = marks.at[0, :heads].set(total).at[1, :heads].set(summit)
    return jnp.concatenate([memory.reshape(heads * rows, width), marks], axis=0)


def unpack_state(packed, heads):
    width = packed.shape[1]
    memory = packed[:-8].reshape(heads, -1, width)
    return packed[-8, :heads], packed[-7, :heads], memory


def carried_in(state, slow, fast):
    total, summit, memory = state
    heads, rows, width = memory.shape
    position = lax.axis_index("sp")
    line, spot = position // fast, position % fast
    slices = memory.reshape(heads, fast, rows // fast, width).transpose(1, 0, 2, 3)

    def own_slice(k):
        return (total, summit, lax.dynamic_index_in_dim(slices, k, 0, keepdims=False))

    packets = [pack_state(own_slice(spot ^ mask)) for mask in range(fast)]
    packets = [packets[0]] + [fast_swap(packets[m], slow, fast, m) for m in range(1, fast)]
    states = [unpack_state(packet, heads) for packet in unswap(packets, spot)]
    nothing = (
        jnp.zeros_like(total),
        jnp.full_like(summit, -1e30),
        jnp.zeros_like(states[0][2]),
    )
    before = [nothing]
    for one in states:
        before.append(join_states(before[-1], one))
    whole = pack_state(before[-1])
    prior = nothing
    for shift in range(slow - 1, 0, -1):
        came = unpack_state(slow_shift(whole, slow, fast, shift, wrap=False), heads)
        joined = join_states(prior, came)
        prior = jax.tree.map(lambda a, b: jnp.where(line >= shift, a, b), joined, prior)
    answers = jnp.stack([pack_state(join_states(prior, one)) for one in before[:-1]])

    def answer(k):
        return lax.dynamic_index_in_dim(answers, k, 0, keepdims=False)

    back = [answer(spot)] + [
        fast_swap(answer(spot ^ mask), slow, fast, mask) for mask in range(1, fast)
    ]
    back = [unpack_state(packet, heads) for packet in unswap(back, spot)]
    return back[0][0], back[0][1], jnp.concatenate([one[2] for one in back], axis=1)


def cell_block(queries, key_rows, values, in_gate, forget_gate, slow, fast):
    highest = lax.Precision.HIGHEST
    tokens_here = queries.shape[0]
    heads = in_gate.shape[0]
    head_dim = queries.shape[1] // heads
    blocks = tokens_here // BLOCK
    key_scale = head_dim ** (-0.5)
    log_forget = jax.nn.log_sigmoid(forget_gate)
    cumulative = jnp.cumsum(log_forget, axis=1)
    total_log = cumulative[:, -1]
    toward = total_log[:, None] - cumulative + in_gate
    summit = jnp.max(toward, axis=1)
    weight_key = jnp.exp(toward - summit[:, None])
    key_scaled = key_rows.astype(jnp.float32).reshape(tokens_here, heads, head_dim) * key_scale
    value_float = values.astype(jnp.float32).reshape(tokens_here, heads, head_dim)
    weighted = key_scaled * weight_key.T[:, :, None]
    memory_dev = jnp.einsum("shd,she->hde", weighted, value_float, precision=highest)
    prior_total, prior_summit, prior_memory = carried_in(
        (total_log, summit, memory_dev), slow, fast
    )
    stabil = jnp.maximum(prior_total, prior_summit)
    memory = jnp.exp(prior_summit - stabil)[:, None, None] * prior_memory
    causal = jnp.tril(jnp.ones((BLOCK, BLOCK), dtype=bool))
    outputs = []
    for block in range(blocks):
        at = slice(block * BLOCK, (block + 1) * BLOCK)
        query_blk = queries[at].reshape(BLOCK, heads, head_dim)
        key_blk = key_rows[at].reshape(BLOCK, heads, head_dim)
        value_blk = values[at].reshape(BLOCK, heads, head_dim)
        input_blk = in_gate[:, at]
        cumul_blk = jnp.cumsum(log_forget[:, at], axis=-1)
        within = jnp.where(
            causal, cumul_blk[:, :, None] - cumul_blk[:, None, :] + input_blk[:, None, :], -jnp.inf
        )
        inner = jnp.max(within, axis=-1)
        raw_scores = (
            jnp.einsum("thd,shd->hts", query_blk, key_blk, preferred_element_type=jnp.float32)
            * key_scale
        )
        probs_low = (raw_scores * jnp.exp(within - inner[:, :, None])).astype(jnp.bfloat16)
        inside = jnp.einsum("hts,shd->thd", probs_low, value_blk, preferred_element_type=jnp.float32)
        across = cumul_blk + stabil[:, None]
        stable = jnp.maximum(across, inner)
        weight_in = jnp.exp(inner - stable)
        weight_out = jnp.exp(across - stable)
        output = weight_in.T[:, :, None] * inside + weight_out.T[:, :, None] * jnp.einsum(
            "thd,hde->the", query_blk.astype(jnp.float32), memory, precision=highest
        )
        outputs.append(output)
        if block + 1 < blocks:
            last_sum = cumul_blk[:, -1]
            toward_blk = last_sum[:, None] - cumul_blk + input_blk
            stabil_new = jnp.maximum(last_sum + stabil, jnp.max(toward_blk, axis=-1))
            weight_blk = jnp.exp(toward_blk - stabil_new[:, None])
            weighted_blk = key_scaled[at] * weight_blk.T[:, :, None]
            memory = jnp.exp(last_sum + stabil - stabil_new)[:, None, None] * memory + jnp.einsum(
                "shd,she->hde", weighted_blk, value_float[at], precision=highest
            )
            stabil = stabil_new
    return jnp.concatenate(outputs, axis=0)


def spread(block_of, slow, fast):
    line = lax.axis_index("sp") // fast
    pieces = [block_of(line)]
    for shift in range(1, slow):
        pieces.append(slow_shift(block_of((line + shift) % slow), slow, fast, shift))
    groups = [list(range(0, slow, 2)), list(range(1, slow, 2))]
    orders = []
    bits = []
    bit = 1
    while bit < fast:
        bits.append(bit)
        bit *= 2
    for route, group in enumerate(groups):
        held = {0: jnp.stack([pieces[s] for s in group])}
        for bit in bits if route == 0 else bits[::-1]:
            for mask in list(held):
                held[mask ^ bit] = fast_swap(held[mask], slow, fast, bit)
        for mask, value in held.items():
            for k, s in enumerate(group):
                orders.append((s, mask, value[k]))
    return orders


def by_source(pieces, slow, fast):
    position = lax.axis_index("sp")
    line, spot = position // fast, position % fast
    first = pieces[0][2]
    whole = jnp.zeros((slow * fast,) + first.shape, first.dtype)
    for shift, mask, value in pieces:
        source = (line - shift) % slow * fast + (spot ^ mask)
        whole = lax.dynamic_update_index_in_dim(whole, value, source, 0)
    return whole


def general(
    stream,
    queries,
    key_rows,
    values,
    out_gate,
    in_gate,
    forget_gate,
    head_gain,
    w_out,
    norm_gains,
    w_gate,
    w_up,
    w_down,
):
    slow, fast = split_axis(lax.axis_size("sp"))
    tokens_here = queries.shape[0]
    own_width = stream.shape[1]
    units = w_gate.shape[1] // slow
    rows_in = w_gate.shape[0]
    columns_out = w_down.shape[1]
    n_sp = slow * fast
    tp_at = lax.axis_index("tp")

    def own_half(value, axis):
        return lax.dynamic_slice_in_dim(value, tp_at * own_width, own_width, axis)

    def column_chunk(weight):
        chunks = weight.reshape(rows_in, slow, units).transpose(1, 0, 2)
        return lambda k: lax.dynamic_index_in_dim(chunks, k, 0, keepdims=False)

    gate_pieces = spread(column_chunk(w_gate), slow, fast)
    up_pieces = spread(column_chunk(w_up), slow, fast)
    down_pieces = spread(
        lambda k: lax.dynamic_slice_in_dim(w_down, k * units, units, 0), slow, fast
    )

    stream_full = tp_gather(stream, 1)
    gains_full = tp_gather(norm_gains, 1).astype(jnp.float32)

    cell = cell_block(queries, key_rows, values, in_gate, forget_gate, slow, fast)
    normed_cell = cell * lax.rsqrt(jnp.mean(cell * cell, axis=-1, keepdims=True) + EPS)
    mixed = (
        normed_cell.reshape(tokens_here, -1)
        * head_gain
        * jax.nn.sigmoid(out_gate.astype(jnp.float32))
    ).astype(jnp.bfloat16)
    partial_mix = jnp.dot(mixed, w_out, preferred_element_type=jnp.float32)
    mix_sum = tp_total(partial_mix.astype(jnp.bfloat16))
    mix_norm = (
        mix_sum
        * lax.rsqrt(jnp.mean(mix_sum * mix_sum, axis=1, keepdims=True) + EPS)
        * gains_full[0]
    )
    after_mix = (stream_full.astype(jnp.float32) + mix_norm).astype(jnp.bfloat16)
    kept_rows = after_mix.astype(jnp.float32)
    normed = (
        kept_rows
        * lax.rsqrt(jnp.mean(kept_rows * kept_rows, axis=1, keepdims=True) + EPS)
        * gains_full[1]
    ).astype(jnp.bfloat16)

    normed_half = own_half(normed, 1)
    arrived = [slow_shift(normed_half, slow, fast, shift) for shift in range(1, slow)]
    others = tp_gather(jnp.concatenate(arrived, axis=0), 1)
    normed_all = jnp.concatenate([normed, others], axis=0)

    gate_rows = by_source(gate_pieces, slow, fast).reshape(n_sp * rows_in, units)
    up_rows = by_source(up_pieces, slow, fast).reshape(n_sp * rows_in, units)
    down_rows = by_source(down_pieces, slow, fast)
    gate_part = jnp.dot(normed_all, gate_rows, preferred_element_type=jnp.float32)
    up_part = jnp.dot(normed_all, up_rows, preferred_element_type=jnp.float32)
    hidden = (jax.nn.silu(gate_part) * up_part).astype(jnp.bfloat16)
    down_full = down_rows.transpose(1, 0, 2).reshape(units, n_sp * columns_out)
    ffn_terms = jnp.dot(hidden, down_full, preferred_element_type=jnp.float32)
    ffn_lines = tp_scatter(ffn_terms.astype(jnp.bfloat16), 1)
    ffn_low = ffn_lines.astype(jnp.bfloat16)
    ffn_sum = ffn_lines[:tokens_here]
    for shift in range(1, slow):
        block = ffn_low[shift * tokens_here : (shift + 1) * tokens_here]
        ffn_sum = ffn_sum + slow_shift(block, slow, fast, -shift).astype(jnp.float32)
    ffn_squares = lax.psum(jnp.sum(ffn_sum * ffn_sum, axis=1), "tp")
    width = own_width * lax.axis_size("tp")
    ffn_norm = (
        ffn_sum
        * lax.rsqrt(ffn_squares / width + EPS)[:, None]
        * norm_gains[2].astype(jnp.float32)
    )
    return (own_half(kept_rows, 1) + 0.5 * ffn_norm).astype(jnp.bfloat16)


LANES = 128
HIGHEST = lax.Precision.HIGHEST


def run(body, outs, *args, spaces=None, scratch=(), flops=10**8, touched=10**7):
    spaces = spaces or {}
    specs = [pl.BlockSpec(memory_space=pltpu.SMEM)] + [
        pl.BlockSpec(memory_space=spaces.get(i, pltpu.VMEM)) for i in range(1, len(args))
    ]
    return pl.pallas_call(
        body,
        out_shape=tuple(jax.ShapeDtypeStruct(shape, kind) for shape, kind in outs),
        in_specs=specs,
        out_specs=tuple(pl.BlockSpec(memory_space=pltpu.VMEM) for _ in outs),
        scratch_shapes=list(scratch),
        cost_estimate=pl.CostEstimate(flops=flops, bytes_accessed=touched, transcendentals=0),
    )(*args)


def aligned(start, size, unit):
    return pl.ds(pl.multiple_of(start, unit), size)


def pack_kernel(slow, full, place, gate, up, down, *packets):
    line = place[0]
    wide = full * LANES
    lanes = lax.broadcasted_iota(jnp.int32, (gate.shape[0], LANES), 1)
    for shift, packet in enumerate(packets):
        chunk = (line + shift) % slow
        for i in range(full):
            columns = aligned(chunk * wide + i * LANES, LANES, LANES)
            packet[:, 2 * i * LANES : (2 * i + 1) * LANES] = gate[:, columns]
            packet[:, (2 * i + 1) * LANES : (2 * i + 2) * LANES] = up[:, columns]
        rest = aligned((slow * full + chunk // 2) * LANES, LANES, LANES)
        gate_rest = gate[:, rest].astype(jnp.float32)
        up_rest = up[:, rest].astype(jnp.float32)
        odd = chunk % 2 == 1
        first = jnp.where(odd, pltpu.roll(gate_rest, LANES // 2, 1), gate_rest)
        second = jnp.where(odd, up_rest, pltpu.roll(up_rest, LANES // 2, 1))
        joint = jnp.where(lanes < LANES // 2, first, second)
        base = (2 * full + 1) * LANES
        packet[:, base - LANES : base] = joint.astype(packet.dtype)
        for i in range(full):
            rows = aligned(chunk * wide + i * LANES, LANES, LANES)
            packet[:, base + i * LANES : base + (i + 1) * LANES] = down[rows, :]
        rows = aligned(slow * wide + chunk * (LANES // 2), LANES // 2, LANES // 2)
        tail = slice(base + full * LANES, base + (full + 1) * LANES)
        packet[: LANES // 2, tail] = down[rows, :]
        packet[LANES // 2 :, tail] = jnp.zeros((LANES // 2, LANES), packet.dtype)


def gate_sums(forget):
    log_forget = -(jnp.maximum(-forget, 0.0) + jnp.log1p(jnp.exp(-jnp.abs(forget))))
    size = forget.shape[1]
    upto = lax.broadcasted_iota(jnp.int32, (size, size), 0) <= lax.broadcasted_iota(
        jnp.int32, (size, size), 1
    )
    return jnp.dot(log_forget, upto.astype(jnp.float32), precision=HIGHEST)


def state_kernel(heads, fast, place, keys, values, in_gate, forget, *rest):
    packets, memory = rest[:-1], rest[-1]
    spot = place[1]
    size = keys.shape[1] // heads
    part = size // fast
    sums = gate_sums(forget[...])
    total = sums[:, -1:]
    toward = total - sums + in_gate[...]
    summit = jnp.max(toward, axis=1, keepdims=True)
    weight = jnp.exp(toward - summit).T * size ** (-0.5)
    for h in range(heads):
        at = slice(h * size, (h + 1) * size)
        weighted = keys[:, at].astype(jnp.float32) * weight[:, h : h + 1]
        memory[h] = jnp.dot(weighted.T, values[:, at].astype(jnp.float32), precision=HIGHEST)
    for mask, packet in enumerate(packets):
        rows = aligned((spot ^ mask) * part, part, part)
        for h in range(heads):
            packet[h * part : (h + 1) * part, :] = memory[h, rows, :]
        base = heads * part
        packet[base : base + heads, :] = jnp.broadcast_to(total, (heads, size))
        packet[base + heads : base + 2 * heads, :] = jnp.broadcast_to(summit, (heads, size))


def open_packet(packet, heads):
    base = packet.shape[0] - 2 * heads
    part = base // heads
    memory = [packet[h * part : (h + 1) * part] for h in range(heads)]
    return packet[base : base + heads], packet[base + heads :], memory


def join_packets(early, late, heads):
    total_early, summit_early, memory_early = early
    total_late, summit_late, memory_late = late
    summit = jnp.maximum(total_late + summit_early, summit_late)
    scale_early = jnp.exp(total_late + summit_early - summit)
    scale_late = jnp.exp(summit_late - summit)
    memory = [
        scale_early[h : h + 1] * memory_early[h] + scale_late[h : h + 1] * memory_late[h]
        for h in range(heads)
    ]
    return total_early + total_late, summit, memory


def empty_packet(heads, shape):
    part = shape[0] // heads - 2
    return (
        jnp.zeros((heads, shape[1]), jnp.float32),
        jnp.full((heads, shape[1]), -1e30, jnp.float32),
        [jnp.zeros((part, shape[1]), jnp.float32)] * heads,
    )


def close_packet(state):
    total, summit, memory = state
    return jnp.concatenate(list(memory) + [total, summit], axis=0)


def plane_kernel(heads, fast, place, *refs):
    came, before, whole, sorted_ = refs[:fast], refs[fast], refs[fast + 1], refs[fast + 2]
    spot = place[1]
    for mask, packet in enumerate(came):
        sorted_[spot ^ mask] = packet[...]
    state = empty_packet(heads, came[0].shape)
    for j in range(fast):
        before[j] = close_packet(state)
        state = join_packets(state, open_packet(sorted_[j], heads), heads)
    whole[...] = close_packet(state)


def line_kernel(heads, slow, fast, place, before, *refs):
    came, answers = refs[: slow - 1], refs[slow - 1 :]
    line, spot = place[0], place[1]
    prior = empty_packet(heads, came[0].shape)
    for shift in range(slow - 1, 0, -1):
        joined = join_packets(prior, open_packet(came[shift - 1][...], heads), heads)
        prior = jax.tree.map(lambda a, b: jnp.where(line >= shift, a, b), joined, prior)
    for mask, answer in enumerate(answers):
        late = open_packet(before[spot ^ mask], heads)
        answer[...] = close_packet(join_packets(prior, late, heads))


def inside_kernel(heads, place, queries, keys, values, in_gate, forget, inside, marks):
    size = keys.shape[1] // heads
    count = keys.shape[0]
    sums = gate_sums(forget[...])
    columns = sums.T
    causal = lax.broadcasted_iota(jnp.int32, (count, count), 1) <= lax.broadcasted_iota(
        jnp.int32, (count, count), 0
    )
    gates = in_gate[...] - sums
    for h in range(heads):
        at = slice(h * size, (h + 1) * size)
        within = jnp.where(causal, columns[:, h : h + 1] + gates[h : h + 1, :], -jnp.inf)
        inner = jnp.max(within, axis=1, keepdims=True)
        raw = lax.dot_general(
            queries[:, at], keys[:, at], (((1,), (1,)), ((), ())), preferred_element_type=jnp.float32
        ) * size ** (-0.5)
        probs = (raw * jnp.exp(within - inner)).astype(jnp.bfloat16)
        inside[:, at] = jnp.dot(probs, values[:, at], preferred_element_type=jnp.float32)
        marks[:, h : h + 1] = inner
        marks[:, heads + h : heads + h + 1] = columns[:, h : h + 1]


def output_kernel(heads, fast, place, queries, inside, marks, out_gate, gain, w_out, *refs):
    back, (partial, memory, weights, mixed, sem) = refs[:fast], refs[fast:]
    spot = place[1]
    size = queries.shape[1] // heads
    part = size // fast
    load = pltpu.make_async_copy(w_out, weights, sem)
    load.start()
    base = heads * part
    total = back[0][base : base + heads, :]
    summit = back[0][base + heads : base + 2 * heads, :]
    stabil = jnp.maximum(total, summit)
    carry = jnp.exp(summit - stabil)
    for mask, packet in enumerate(back):
        rows = aligned((spot ^ mask) * part, part, part)
        for h in range(heads):
            memory[h, rows, :] = packet[h * part : (h + 1) * part, :] * carry[h : h + 1]
    for h in range(heads):
        at = slice(h * size, (h + 1) * size)
        inner = marks[:, h : h + 1]
        across = marks[:, heads + h : heads + h + 1] + stabil[h : h + 1, :]
        stable = jnp.maximum(across, inner)
        carried = jnp.dot(queries[:, at].astype(jnp.float32), memory[h], precision=HIGHEST)
        cell = jnp.exp(inner - stable) * inside[:, at] + jnp.exp(across - stable) * carried
        scale = lax.rsqrt(jnp.mean(cell * cell, axis=1, keepdims=True) + EPS)
        opened = 1.0 / (1.0 + jnp.exp(-out_gate[:, at].astype(jnp.float32)))
        mixed[:, at] = (cell * scale * gain[:, at] * opened).astype(jnp.bfloat16)
    load.wait()
    step = 4 * LANES

    @pl.loop(0, weights.shape[1] // step)
    def _(i):
        columns = aligned(i * step, step, step)
        partial[:, columns] = jnp.dot(
            mixed[...], weights[:, columns], preferred_element_type=jnp.float32
        ).astype(jnp.bfloat16)


def norm_kernel(place, own, other, stream, gains, normed, half, kept):
    width = half.shape[1]
    mine = aligned(place[2] * width, width, width)
    count = own.shape[1]
    mix = own[...].astype(jnp.float32) + other[...].astype(jnp.float32)
    scale = lax.rsqrt(jnp.sum(mix * mix, axis=1, keepdims=True) / count + EPS)
    after = (stream[...].astype(jnp.float32) + mix * scale * gains[0:1, :]).astype(jnp.bfloat16)
    rows = after.astype(jnp.float32)
    scale = lax.rsqrt(jnp.sum(rows * rows, axis=1, keepdims=True) / count + EPS)
    normed[...] = (rows * scale * gains[1:2, :]).astype(jnp.bfloat16)
    half[...] = normed[:, mine]
    first = place[2] == 0
    kept[...] = jnp.where(first, rows[:, :width], rows[:, width:]).astype(jnp.bfloat16)


def ffn_kernel(slow, fast, full, place, *refs):
    count = slow * fast
    normed, near, far = refs[0], refs[1:slow], refs[slow : 2 * slow - 1]
    pieces = refs[2 * slow - 1 : 2 * slow - 1 + count]
    send, keep, rows_in, wide, narrow, hidden, sems = refs[2 * slow - 1 + count :]
    line, spot, side = place[0], place[1], place[2]
    tokens, width = near[0].shape
    base = (2 * full + 1) * LANES
    units = full * LANES + LANES // 2
    first, second, third = [], [], []
    first.append(pltpu.make_async_copy(normed, rows_in.at[pl.ds(0, tokens), :], sems.at[0]))
    for s in range(1, slow):
        at = pl.ds(s * tokens, tokens)
        for source, half in ((near[s - 1], side), (far[s - 1], 1 - side)):
            place_at = rows_in.at[at, aligned(half * width, width, width)]
            first.append(pltpu.make_async_copy(source, place_at, sems.at[0]))
    for s in range(slow):
        for mask in range(fast):
            piece = pieces[s * fast + mask]
            source = (line + slow - s) % slow * fast + (spot ^ mask)
            at = aligned(source * LANES, LANES, LANES)
            second.append(
                pltpu.make_async_copy(piece.at[:, pl.ds(0, base)], wide.at[at, :], sems.at[1])
            )
            for i in range(full + 1):
                depth = LANES if i < full else LANES // 2
                third.append(
                    pltpu.make_async_copy(
                        piece.at[pl.ds(0, depth), pl.ds(base + i * LANES, LANES)],
                        narrow.at[pl.ds(i * LANES, depth), at],
                        sems.at[2],
                    )
                )
    for copy in first + second + third:
        copy.start()
    for copy in first + second:
        copy.wait()

    def act(gate, up):
        return (gate / (1.0 + jnp.exp(-gate)) * up).astype(jnp.bfloat16)

    @pl.loop(0, full)
    def _(i):
        both = jnp.dot(
            rows_in[...],
            wide[:, aligned(i * 2 * LANES, 2 * LANES, 2 * LANES)],
            preferred_element_type=jnp.float32,
        )
        hidden[:, aligned(i * LANES, LANES, LANES)] = act(both[:, :LANES], both[:, LANES:])

    both = jnp.dot(rows_in[...], wide[:, base - LANES :], preferred_element_type=jnp.float32)
    hidden[:, full * LANES :] = act(both, pltpu.roll(both, LANES // 2, 1))[:, : LANES // 2]
    for copy in third:
        copy.wait()
    step = 2 * LANES

    def product(half, i):
        columns = aligned(half * width + i * step, step, step)
        return jnp.dot(hidden[...], narrow[:, columns], preferred_element_type=jnp.float32)

    @pl.loop(0, width // step)
    def _(i):
        send[:, aligned(i * step, step, step)] = product(1 - side, i).astype(jnp.bfloat16)
        keep[:, aligned(i * step, step, step)] = product(side, i)


def share_kernel(place, keep, came, own, *parts):
    tokens = own.shape[0]
    own[...] = keep[:tokens, :] + came[:tokens, :].astype(jnp.float32)
    for s, part in enumerate(parts):
        at = slice((s + 1) * tokens, (s + 2) * tokens)
        part[...] = (keep[at, :] + came[at, :].astype(jnp.float32)).astype(jnp.bfloat16)


def other_core(value):
    return lax.ppermute(value, "tp", [(0, 1), (1, 0)])


def fitted(
    stream,
    queries,
    key_rows,
    values,
    out_gate,
    in_gate,
    forget_gate,
    head_gain,
    w_out,
    norm_gains,
    w_gate,
    w_up,
    w_down,
):
    bf16, f32 = jnp.bfloat16, jnp.float32
    slow, fast = split_axis(lax.axis_size("sp"))
    tokens, width = stream.shape
    heads = in_gate.shape[0]
    size = queries.shape[1] // heads
    part = size // fast
    full = w_gate.shape[1] // slow // LANES
    units = w_gate.shape[1] // slow
    position = lax.axis_index("sp")
    place = jnp.stack([position // fast, position % fast, lax.axis_index("tp")]).astype(jnp.int32)
    any_space = pl.ANY

    packets = run(
        lambda *refs: pack_kernel(slow, full, *refs),
        [((LANES, (3 * full + 2) * LANES), bf16)] * slow,
        place, w_gate, w_up, w_down,
    )
    state_shape = (heads * (part + 2), size)
    states = run(
        lambda *refs: state_kernel(heads, fast, *refs),
        [(state_shape, f32)] * fast,
        place, key_rows, values, in_gate, forget_gate,
        scratch=[pltpu.VMEM((heads, size, size), f32)],
    )

    pieces = [packets[0]] + [slow_shift(packets[s], slow, fast, s) for s in range(1, slow)]
    bits = [1 << b for b in range(fast.bit_length() - 1)]
    weights = []
    for s, piece in enumerate(pieces):
        held = {0: piece}
        for bit in bits if s % 2 == 0 else bits[::-1]:
            for mask in list(held):
                held[mask ^ bit] = fast_swap(held[mask], slow, fast, bit)
        weights += [held[mask] for mask in range(fast)]

    states = [states[0]] + [fast_swap(states[m], slow, fast, m) for m in range(1, fast)]
    before, whole = run(
        lambda *refs: plane_kernel(heads, fast, *refs),
        [((fast,) + state_shape, f32), (state_shape, f32)],
        place, *states,
        scratch=[pltpu.VMEM((fast,) + state_shape, f32)],
    )
    earlier = [slow_shift(whole, slow, fast, s, wrap=False) for s in range(1, slow)]
    answers = run(
        lambda *refs: line_kernel(heads, slow, fast, *refs),
        [(state_shape, f32)] * fast,
        place, before, *earlier,
    )
    answers = [answers[0]] + [fast_swap(answers[m], slow, fast, m) for m in range(1, fast)]

    inside, marks = run(
        lambda *refs: inside_kernel(heads, *refs),
        [((tokens, heads * size), f32), ((tokens, 2 * heads), f32)],
        place, queries, key_rows, values, in_gate, forget_gate,
    )
    stream_full = tp_gather(stream, 1)
    gains_full = tp_gather(norm_gains, 1).astype(f32)
    (partial,) = run(
        lambda *refs: output_kernel(heads, fast, *refs),
        [((tokens, 2 * width), bf16)],
        place, queries, inside, marks, out_gate, head_gain[None, :], w_out, *answers,
        spaces={6: any_space},
        scratch=[
            pltpu.VMEM((heads, size, size), f32),
            pltpu.VMEM(w_out.shape, bf16),
            pltpu.VMEM((tokens, heads * size), bf16),
            pltpu.SemaphoreType.DMA,
        ],
    )
    normed, half, kept = run(
        norm_kernel,
        [((tokens, 2 * width), bf16), ((tokens, width), bf16), ((tokens, width), bf16)],
        place, partial, other_core(partial), stream_full, gains_full,
    )
    near = [slow_shift(half, slow, fast, s) for s in range(1, slow)]
    far = [other_core(value) for value in near]
    count = 1 + 2 * (slow - 1) + slow * fast
    send, keep = run(
        lambda *refs: ffn_kernel(slow, fast, full, *refs),
        [((slow * tokens, width), bf16), ((slow * tokens, width), f32)],
        place, normed, *near, *far, *weights,
        spaces={i: any_space for i in range(1, count + 1)},
        scratch=[
            pltpu.VMEM((slow * tokens, 2 * width), bf16),
            pltpu.VMEM((2 * width, (2 * full + 1) * LANES), bf16),
            pltpu.VMEM((units, 2 * width), bf16),
            pltpu.VMEM((slow * tokens, units), bf16),
            pltpu.SemaphoreType.DMA((3,)),
        ],
        flops=4 * 10**9,
    )
    shares = run(
        share_kernel,
        [((tokens, width), f32)] + [((tokens, width), bf16)] * (slow - 1),
        place, keep, other_core(send),
    )
    ffn_sum = shares[0]
    for s in range(1, slow):
        ffn_sum = ffn_sum + slow_shift(shares[s], slow, fast, -s).astype(f32)
    ffn_squares = lax.psum(jnp.sum(ffn_sum * ffn_sum, axis=1), "tp")
    ffn_norm = (
        ffn_sum
        * lax.rsqrt(ffn_squares / (2 * width) + EPS)[:, None]
        * norm_gains[2].astype(f32)
    )
    return (kept.astype(f32) + 0.5 * ffn_norm).astype(bf16)


def shards(*args):
    slow, fast = split_axis(lax.axis_size("sp"))
    tokens, width = args[0].shape
    heads = args[5].shape[0]
    w_gate, w_down = args[10], args[12]
    fits = (
        lax.axis_size("tp") == 2
        and fast & (fast - 1) == 0
        and slow % 2 == 0
        and tokens == LANES
        and args[1].shape[1] == heads * LANES
        and heads % 8 == 0
        and width % (4 * LANES) == 0
        and w_gate.shape[0] == LANES
        and w_down.shape[1] == LANES
        and w_gate.shape[1] // slow % LANES == LANES // 2
        and LANES // fast % 8 == 0
    )
    return (fitted if fits else general)(*args)


def solution(mesh):
    in_specs = (
        P("sp", "tp"),
        P("sp", "tp"),
        P("sp", "tp"),
        P("sp", "tp"),
        P("sp", "tp"),
        P("tp", "sp"),
        P("tp", "sp"),
        P("tp"),
        P("tp", None),
        P(None, "tp"),
        P("sp", "tp"),
        P("sp", "tp"),
        P("tp", "sp"),
    )
    out_specs = P("sp", "tp")
    return jax.shard_map(shards, mesh=mesh, in_specs=in_specs, out_specs=out_specs, check_vma=False)
```
